32 devices in a mesh: ep: 8 (over z, x), tp: 4 (over y, core).
Axes of the slice: x: 2, y: 2, z: 4, core: 2. Of those that a mesh axis runs over, the one named last changes fastest.
Arguments:
- tokens: bfloat16 [128, 2048], P('ep'), may hold values from -120 to 120
- lengths: int32 [128], P('ep'), may hold values from 1 to 768, as said below
- cache_kv: bfloat16 [128, 768, 16, 128], P('ep', None, 'tp'), may hold values from -64 to 64
- cache_cum: float32 [128, 16, 768], P('ep', 'tp'), may hold values from -768 to 0, as said below
- norm_attn: float32 [2048], replicated, may hold values from 0.1 to 1.9
- w_query: bfloat16 [2048, 1024], P(None, 'tp'), may hold values from -0.125 to 0.125
- w_key: bfloat16 [2048, 1024], P(None, 'tp'), may hold values from -0.125 to 0.125
- w_value: bfloat16 [2048, 1024], P(None, 'tp'), may hold values from -0.125 to 0.125
- w_forget: bfloat16 [2048, 16], P(None, 'tp'), may hold values from -0.125 to 0.125
- b_forget: float32 [16], P('tp'), may hold values from -1 to 2
- w_output: bfloat16 [1024, 2048], P('tp'), may hold values from -0.1875 to 0.1875
- norm_ffn: float32 [2048], replicated, may hold values from 0.1 to 1.9
- shared_gate: bfloat16 [2048, 512], P(None, 'tp'), may hold values from -0.125 to 0.125
- shared_up: bfloat16 [2048, 512], P(None, 'tp'), may hold values from -0.125 to 0.125
- shared_down: bfloat16 [512, 2048], P('tp'), may hold values from -0.25 to 0.25
- expert_gate: bfloat16 [24, 2048, 512], P('ep', None, 'tp'), may hold values from -0.125 to 0.125
- expert_up: bfloat16 [24, 2048, 512], P('ep', None, 'tp'), may hold values from -0.125 to 0.125
- expert_down: bfloat16 [24, 512, 2048], P('ep', 'tp'), may hold values from -0.25 to 0.25
- route_ids: int32 [128, 6], P('ep'), may hold values from 0 to 23, all different within a row; in each aligned block of 16 rows (0 to 15, 16 to 31, ...) at most 8 rows name the same one
- route_weight: float32 [128, 6], P('ep'), may hold values from 0.1 to 0.8
Outputs:
- output: bfloat16 [128, 2048], P('ep', 'tp')
- new_kv: bfloat16 [128, 16, 128], P('ep', 'tp')
- new_cum: float32 [128, 16], P('ep', 'tp')
The draws below stay inside these ranges and needn't reach their ends.
Inputs may be any that keep to these rules, and one draw needn't show every extreme that they name: `lengths`: every block of 16 sequences of one index of ep holds one with 768. `route_ids`: in the rows of one device (aligned blocks of 16 rows) no expert is named more than 8 times. `cache_cum`: Non-increasing along positions.
All inputs are finite; a program needn't handle non-finite values.
Results may differ from the reference program's by a relative error of at most 0.012.
Values may be sent and summed in bfloat16 or wider, within the bound.
A program may use at most 128 MiB of HBM per device.

```python
import math
import jax
import jax.numpy as jnp
import numpy as np
from jax import lax

D = 2048
ATTENTION_HEADS = 16
HEAD_DIM = 64
EF = 512
SF = 512
TOPK = 6
SEQ_DEV = 16
CACHE_POSITIONS = 768
SEQUENCE_COUNT = 128
EXPERTS = 24
CAP = 8
N_EP = 8
N_TP = 4


def length_draw(key):
    base_key = jax.random.fold_in(key, 11)
    drawn = jax.random.randint(base_key, (SEQUENCE_COUNT,), 1, CACHE_POSITIONS + 1)
    filled = jnp.arange(SEQUENCE_COUNT, dtype=jnp.int32) % SEQ_DEV == 0
    return jnp.where(filled, CACHE_POSITIONS, drawn).astype(jnp.int32)


def draw_lengths(key, part):
    return length_draw(key)


def draw_tokens(key, part):
    column_key = jax.random.fold_in(key, 41)
    row_key = jax.random.fold_in(key, 42)
    noise_key = jax.random.fold_in(key, 43)
    columns = jnp.arange(D, dtype=jnp.float32)
    column_scale = 0.3 * jnp.exp(jnp.log(10.0) * columns / D) * jnp.exp(jax.random.uniform(column_key, (D,), jnp.float32, -0.7, 0.7))
    row_scale = jnp.exp(jax.random.uniform(row_key, (SEQUENCE_COUNT, 1), jnp.float32, jnp.log(0.3), jnp.log(3.0)))
    noise_draw = jnp.clip(jax.random.normal(noise_key, (SEQUENCE_COUNT, D), jnp.float32), -6.0, 6.0)
    return (noise_draw * row_scale * column_scale[None, :]).astype(jnp.bfloat16)


def draw_cache_kv(key, part):
    noise_key = jax.random.fold_in(key, 21)
    shape = (SEQUENCE_COUNT, CACHE_POSITIONS, ATTENTION_HEADS, 2 * HEAD_DIM)
    values = jnp.clip(jax.random.normal(noise_key, shape, jnp.float32), -6.0, 6.0)
    return values.astype(jnp.bfloat16)


def draw_cache_cum(key, part):
    head_key = jax.random.fold_in(key, 31)
    factor_key = jax.random.fold_in(key, 32)
    rough_key = jax.random.fold_in(key, 33)
    spike_random_key = jax.random.fold_in(key, 34)
    height_random_key = jax.random.fold_in(key, 35)
    slow_share = 0.5
    slow = jax.random.uniform(head_key, (SEQUENCE_COUNT, ATTENTION_HEADS)) < slow_share
    seq_factor = jnp.exp(jax.random.uniform(factor_key, (SEQUENCE_COUNT, 1), jnp.float32, -0.7, 0.7))
    falloff_speed = jnp.where(slow, 0.5 / CACHE_POSITIONS, 1.0 / 40.0) * seq_factor
    jaggedness = jnp.exp(jax.random.uniform(rough_key, (SEQUENCE_COUNT, ATTENTION_HEADS, CACHE_POSITIONS), jnp.float32, -1.1, 1.1))
    spike_mask = jax.random.uniform(spike_random_key, (SEQUENCE_COUNT, ATTENTION_HEADS, CACHE_POSITIONS)) < 2.0 / CACHE_POSITIONS
    spike_height = jax.random.uniform(height_random_key, (SEQUENCE_COUNT, ATTENTION_HEADS, CACHE_POSITIONS), jnp.float32, 0.22, 0.69)
    stride_amounts = falloff_speed[:, :, None] * jaggedness + jnp.where(spike_mask, spike_height, 0.0)
    return -jnp.cumsum(stride_amounts, axis=2)


def level_of(rng, shape, cuts, low, top_value):
    loudness, own = 1.0, jax.random.fold_in(rng, 6)
    for position, parts in cuts:
        draws = jnp.exp(jax.random.uniform(jax.random.fold_in(own, position), (parts,), jnp.float32, low / len(cuts), top_value / len(cuts)))
        loudness = loudness * jnp.repeat(draws, shape[position] // parts).reshape([-1 if axis == position else 1 for axis in range(len(shape))])
    return loudness


def assign_block(key, own, number, rows, count, top, reach, lean):
    ranking = jax.random.permutation(key, count)
    heavy_load, common = shares(count, rows * top, reach, lean, True), shares(count, rows * top, reach, lean, False)
    places = jnp.arange(count)

    def named(tallies, offset_by):
        used = int((tallies > 0).sum())
        fixed = max(1, used // 4)
        shifted = fixed + (places - fixed + offset_by * (used - fixed)) % max(1, count - fixed)
        return jnp.zeros((count,), jnp.int32).at[ranking[jnp.where(places < fixed, places, shifted)]].set(jnp.asarray(tallies, jnp.int32))

    tallies = jnp.where(number % 4 == 0, named(heavy_load, number // 4), named(common, number - number // 4 - 1))
    mixed = jax.random.permutation(jax.random.fold_in(own, 3), count)
    source_of, taker = mixed[0:count // 2 * 2:2], mixed[1:count // 2 * 2:2]
    margin = jnp.minimum(tallies[source_of] - 1, reach - tallies[taker]) // 2
    margin = jnp.where((source_of == ranking[0]) | (taker == ranking[0]) | (tallies[taker] == 0), 0, jnp.maximum(margin, 0))
    shifted = jax.random.randint(jax.random.fold_in(own, 4), (count // 2,), 0, 1 << 20) % (margin + 1)
    tallies = tallies.at[source_of].add(-shifted).at[taker].add(shifted)
    items = jnp.searchsorted(jnp.cumsum(tallies), jnp.arange(rows * top), side="right").astype(jnp.int32)
    listing = items.reshape(top, rows).T
    listing = listing[jax.random.permutation(jax.random.fold_in(own, 1), rows)]
    offset_by = jax.random.randint(jax.random.fold_in(own, 2), (rows, 1), 0, top)
    return jnp.take_along_axis(listing, (jnp.arange(top)[None, :] + offset_by) % top, axis=1)


def shares(amount, total, limit, slope, full):
    weights = [(1 << 20) // math.isqrt(standing ** slope) + 1 for standing in range(1, amount + 1)]
    largest = limit if full else min(limit, max(-(-total // amount), total * weights[0] // sum(weights)))
    least = 1 if total - largest >= amount - 1 else 0
    given, spare = [largest] + [least] * (amount - 1), total - largest - least * (amount - 1)
    while spare > 0:
        candidates = [i for i in range(1, amount) if given[i] < largest] or [i for i in range(1, amount) if given[i] < limit]
        pool, remaining = sum([weights[i] for i in candidates]), spare
        for i in candidates:
            more = min(limit - given[i], max(1, remaining * weights[i] // pool), spare)
            given[i] = given[i] + more
            spare = spare - more
    return np.array(given)


def normal_values(rng, dims, width, limit, shards=(), kind=jnp.bfloat16):
    values = jax.random.normal(rng, dims, jnp.float32) * width
    if len(shards) > 0:
        values = level_of(rng, dims, shards, -0.22, 0.18) * values
    return jnp.clip(values, min=-limit, max=limit).astype(kind)


def setup_inputs(seed: int = 0) -> dict:
    key_of = jax.random.split(jax.random.key(seed), 21)
    tokens = draw_tokens(jax.random.fold_in(key_of[20], 71), 0)
    lengths = draw_lengths(jax.random.fold_in(key_of[20], 71), 0)
    cache_kv = draw_cache_kv(jax.random.fold_in(key_of[20], 71), 0)
    cache_cum = draw_cache_cum(jax.random.fold_in(key_of[20], 71), 0)
    norm_attn = jnp.clip(1.0 + 0.18 * jax.random.normal(key_of[4], (D,), jnp.float32), 0.1, 1.9)
    w_query = normal_values(key_of[5], (D, ATTENTION_HEADS * HEAD_DIM), D ** -0.5, 0.125, ((1, 4),))
    w_key = normal_values(key_of[6], (D, ATTENTION_HEADS * HEAD_DIM), D ** -0.5, 0.125, ((1, 4),))
    w_value = normal_values(key_of[7], (D, ATTENTION_HEADS * HEAD_DIM), D ** -0.5, 0.125, ((1, 4),))
    w_forget = normal_values(key_of[8], (D, ATTENTION_HEADS), D ** -0.5, 0.125, ((1, 4),))
    b_forget = jnp.clip(-1.0 + 3.0 * jax.random.uniform(key_of[9], (ATTENTION_HEADS,), jnp.float32) ** level_of(key_of[9], (ATTENTION_HEADS,), ((0, 4),), -0.2, 0.2), -1.0, 2.0)
    w_output = normal_values(key_of[10], (ATTENTION_HEADS * HEAD_DIM, D), (ATTENTION_HEADS * HEAD_DIM) ** -0.5, 0.1875, ((0, 4),))
    norm_ffn = jnp.clip(1.0 + 0.18 * jax.random.normal(key_of[11], (D,), jnp.float32), 0.1, 1.9)
    shared_gate = normal_values(key_of[12], (D, SF), D ** -0.5, 0.125, ((1, 4),))
    shared_up = normal_values(key_of[13], (D, SF), D ** -0.5, 0.125, ((1, 4),))
    shared_down = normal_values(key_of[14], (SF, D), SF ** -0.5, 0.25, ((0, 4),))
    expert_gate = normal_values(key_of[15], (EXPERTS, D, EF), D ** -0.5, 0.125, ((0, 8), (2, 4)))
    expert_up = normal_values(key_of[16], (EXPERTS, D, EF), D ** -0.5, 0.125, ((0, 8), (2, 4)))
    expert_down = normal_values(key_of[17], (EXPERTS, EF, D), EF ** -0.5, 0.25, ((0, 8), (1, 4)))
    route_ids_keys = jax.random.split(jax.random.fold_in(key_of[18], 1), SEQUENCE_COUNT // SEQ_DEV)
    route_ids_turns = jax.random.permutation(jax.random.fold_in(key_of[18], 3), SEQUENCE_COUNT // SEQ_DEV)
    route_ids = jax.vmap(lambda own, number: assign_block(jax.random.fold_in(key_of[18], 2), own, number, SEQ_DEV, EXPERTS, TOPK, CAP, 1))(route_ids_keys, route_ids_turns).reshape((SEQUENCE_COUNT, TOPK))
    route_weight = jnp.clip(jnp.exp(math.log(0.8) - 2.0794415 * jax.random.uniform(key_of[19], (SEQUENCE_COUNT, TOPK), jnp.float32) ** level_of(key_of[19], (SEQUENCE_COUNT, TOPK), ((0, 8),), -0.2, 0.2)), 0.1, 0.8)
    return {"tokens": tokens, "lengths": lengths, "cache_kv": cache_kv, "cache_cum": cache_cum, "norm_attn": norm_attn, "w_query": w_query, "w_key": w_key, "w_value": w_value, "w_forget": w_forget, "b_forget": b_forget, "w_output": w_output, "norm_ffn": norm_ffn, "shared_gate": shared_gate, "shared_up": shared_up, "shared_down": shared_down, "expert_gate": expert_gate, "expert_up": expert_up, "expert_down": expert_down, "route_ids": route_ids, "route_weight": route_weight}


epsilon = 1e-06

def rms_scale(row_block, gain):
    widened = row_block.astype(jnp.float32)
    return widened * lax.rsqrt(lax.optimization_barrier(jnp.mean(widened * widened, axis=-1, keepdims=True)) + epsilon) * gain

def split_sum(hidden, weight):
    row_count = hidden.shape[0]
    pieces = jnp.einsum('rtf,tfd->rtd', hidden.reshape(row_count, N_TP, -1).astype(jnp.float32), weight.reshape(N_TP, -1, weight.shape[1]).astype(jnp.float32))
    rounded = lax.optimization_barrier(pieces.astype(jnp.bfloat16))
    return lax.optimization_barrier(jnp.sum(rounded.astype(jnp.float32), axis=1))

def expert_apply(row_block, w_gate, w_up, w_down):
    gate_value = jnp.dot(row_block, w_gate, preferred_element_type=jnp.float32)
    up_value = jnp.dot(row_block, w_up, preferred_element_type=jnp.float32)
    hidden = (jax.nn.silu(gate_value) * up_value).astype(jnp.bfloat16)
    return split_sum(hidden, w_down)

def attend_one(inputs):
    queries, key_new, value_new, cache_rows, cum_rows, length, cum_new = inputs
    score_scale = HEAD_DIM ** (-0.5)
    keys_past = cache_rows[:, :, :HEAD_DIM].astype(jnp.float32)
    values_past = cache_rows[:, :, HEAD_DIM:].astype(jnp.float32)
    widened = queries.astype(jnp.float32)
    past_scores = jnp.einsum('hd,lhd->hl', widened, keys_past) * score_scale
    past_scores = past_scores + cum_new[:, None] - cum_rows
    is_valid = jnp.arange(CACHE_POSITIONS, dtype=jnp.int32)[None, :] < length
    past_scores = jnp.where(is_valid, past_scores, -jnp.inf)
    own_score = lax.optimization_barrier(jnp.sum(widened * key_new.astype(jnp.float32), axis=1)) * score_scale
    row_max = jnp.maximum(lax.optimization_barrier(jnp.max(past_scores, axis=1)), own_score)
    weights_past = jnp.exp(past_scores - row_max[:, None])
    weight_own = jnp.exp(own_score - row_max)
    weight_sum = lax.optimization_barrier(jnp.sum(weights_past, axis=1)) + weight_own
    probs_past = (weights_past / weight_sum[:, None]).astype(jnp.bfloat16)
    prob_own = (weight_own / weight_sum).astype(jnp.bfloat16)
    mixed = jnp.einsum('hl,lhd->hd', probs_past.astype(jnp.float32), values_past)
    mixed = mixed + prob_own.astype(jnp.float32)[:, None] * value_new.astype(jnp.float32)
    return mixed.astype(jnp.bfloat16)

def run_expert(inputs):
    return expert_apply(*inputs).astype(jnp.bfloat16)

def reference(tokens, lengths, cache_kv, cache_cum, norm_attn, w_query, w_key, w_value, w_forget, b_forget, w_output, norm_ffn, shared_gate, shared_up, shared_down, expert_gate, expert_up, expert_down, route_ids, route_weight):
    seq_total = tokens.shape[0]
    normed = rms_scale(tokens, norm_attn).astype(jnp.bfloat16)
    queries = jnp.dot(normed, w_query, preferred_element_type=jnp.float32).astype(jnp.bfloat16).reshape(seq_total, ATTENTION_HEADS, HEAD_DIM)
    key_new = jnp.dot(normed, w_key, preferred_element_type=jnp.float32).astype(jnp.bfloat16).reshape(seq_total, ATTENTION_HEADS, HEAD_DIM)
    value_new = jnp.dot(normed, w_value, preferred_element_type=jnp.float32).astype(jnp.bfloat16).reshape(seq_total, ATTENTION_HEADS, HEAD_DIM)
    forget_log = jax.nn.log_sigmoid(jnp.dot(normed, w_forget, preferred_element_type=jnp.float32) + b_forget)
    last_index = jnp.broadcast_to((lengths - 1)[:, None, None], (seq_total, ATTENTION_HEADS, 1)).astype(jnp.int32)
    cum_new = jnp.take_along_axis(cache_cum, last_index, axis=2)[:, :, 0] + forget_log
    attended = lax.map(attend_one, (queries, key_new, value_new, cache_kv, cache_cum, lengths, cum_new))
    attended = attended.reshape(seq_total, ATTENTION_HEADS * HEAD_DIM)
    residual = (tokens.astype(jnp.float32) + split_sum(attended, w_output)).astype(jnp.bfloat16)
    ffn_in = rms_scale(residual, norm_ffn).astype(jnp.bfloat16)
    shared_out = expert_apply(ffn_in, shared_gate, shared_up, shared_down)
    route_flat = route_ids.reshape(N_EP, SEQ_DEV * TOPK)
    onehot = (route_flat[:, :, None] == jnp.arange(EXPERTS, dtype=jnp.int32)[None, None, :]).astype(jnp.int32)
    before = jnp.cumsum(onehot, axis=1) - onehot
    slot_rank = lax.optimization_barrier(jnp.sum(before * onehot, axis=2))
    group_index = jnp.arange(N_EP, dtype=jnp.int32)[:, None]
    slot_index = ((route_flat * N_EP + group_index) * CAP + slot_rank).reshape(-1).astype(jnp.int32)
    token_of_route = jnp.repeat(jnp.arange(seq_total, dtype=jnp.int32), TOPK)
    buffer = jnp.zeros((EXPERTS * N_EP * CAP, D), jnp.bfloat16).at[slot_index].set(ffn_in[token_of_route])
    expert_rows = buffer.reshape(EXPERTS, N_EP * CAP, D)
    expert_out = lax.map(run_expert, (expert_rows, expert_gate, expert_up, expert_down))
    picked = expert_out.reshape(-1, D)[slot_index].reshape(seq_total, TOPK, D).astype(jnp.float32)
    routed = lax.optimization_barrier(jnp.sum(picked * route_weight[:, :, None], axis=1))
    output = (residual.astype(jnp.float32) + shared_out + routed).astype(jnp.bfloat16)
    new_kv = jnp.concatenate([key_new, value_new], axis=2)
    return (output, new_kv, cum_new)
```

```python
import functools

import jax
import jax.numpy as jnp
from jax import lax
from jax.experimental import pallas as pl
from jax.experimental.pallas import tpu as pltpu
from jax.sharding import PartitionSpec as P

HEAD_DIM = 64
LANES = 128
epsilon = 1e-06
MESH = pl.DeviceIdType.MESH
F32 = jnp.float32
BF16 = jnp.bfloat16


def rms_scale(row_block, gain):
    widened = row_block.astype(F32)
    return widened * lax.rsqrt(jnp.mean(widened * widened, axis=-1, keepdims=True) + epsilon) * gain


def attention_kernel(
    group,
    lengths_ref,
    tokens_ref,
    cum_ref,
    gain_ref,
    wf_ref,
    bf_ref,
    wq_hbm,
    wk_hbm,
    wv_hbm,
    wo_hbm,
    kv_hbm,
    partial_ref,
    new_kv_ref,
    new_cum_ref,
    wq,
    wk,
    wv,
    wo,
    kv,
    q_pad,
    fresh,
    forget,
    cum_new,
    mixed_all,
    w_sem,
    kv_sem,
):
    seqs = tokens_ref.shape[0]
    heads = new_kv_ref.shape[1]
    columns = kv.shape[1]
    rows = q_pad.shape[1]
    scale = HEAD_DIM ** (-0.5)
    w_copies = [
        pltpu.make_async_copy(src, dst, w_sem.at[i])
        for i, (src, dst) in enumerate(((wq_hbm, wq), (wk_hbm, wk), (wv_hbm, wv), (wo_hbm, wo)))
    ]

    def kv_copy(s):
        return pltpu.make_async_copy(kv_hbm.at[s], kv.at[s], kv_sem.at[s])

    for copy in w_copies[:3]:
        copy.start()
    for s in range(seqs):
        kv_copy(s).start()
    w_copies[3].start()

    normed = rms_scale(tokens_ref[...], gain_ref[...]).astype(BF16)
    forget_log = jax.nn.log_sigmoid(
        lax.dot_general(
            normed, wf_ref[...], (((1,), (1,)), ((), ())), preferred_element_type=F32
        )
        + bf_ref[...]
    )
    q_pad[...] = jnp.zeros_like(q_pad)
    fresh[...] = jnp.zeros_like(fresh)
    forget[...] = jnp.zeros_like(forget)
    lane = lax.broadcasted_iota(jnp.int32, (seqs, LANES), 1)
    low = lane < HEAD_DIM
    for copy in w_copies[:3]:
        copy.wait()
    queries, keys, values = (
        jnp.dot(normed, w[...], preferred_element_type=F32).astype(BF16).astype(F32)
        for w in (wq, wk, wv)
    )
    for h in range(heads):
        pair = slice((h // 2) * LANES, (h // 2 + 1) * LANES)
        q_h, k_h, v_h = queries[:, pair], keys[:, pair], values[:, pair]
        if h % 2 == 0:
            v_h = pltpu.roll(v_h, HEAD_DIM, 1)
        else:
            q_h = pltpu.roll(q_h, HEAD_DIM, 1)
            k_h = pltpu.roll(k_h, HEAD_DIM, 1)
        q_pad[:, h, :] = jnp.where(low, q_h, 0.0)
        fresh[:, h, :] = jnp.where(low, k_h, v_h)
        forget[:, h, :] = jnp.broadcast_to(forget_log[:, h : h + 1], (seqs, LANES))
    new_kv_ref[...] = fresh[:, :heads, :].astype(BF16)

    column = lax.broadcasted_iota(jnp.int32, (rows, columns), 1)
    own_head = lax.rem(column, heads) == lax.broadcasted_iota(jnp.int32, (rows, columns), 0)

    def attend(s):
        kv_copy(s).wait()
        length = lengths_ref[s]
        rows_kv = kv[s]
        q = q_pad[s]
        new = fresh[s]
        cum = cum_ref[s]
        scores = lax.dot_general(
            q.astype(BF16), rows_kv, (((1,), (1,)), ((), ())), preferred_element_type=F32
        )
        last = own_head & (column >= (length - 1) * heads) & (column < length * heads)
        cum_here = jnp.sum(jnp.where(last, cum, 0.0), axis=1, keepdims=True) + forget[s][:, :1]
        cum_new[s] = jnp.broadcast_to(cum_here, (rows, LANES))
        valid = own_head & (column < length * heads)
        scores = jnp.where(valid, scores * scale + cum_here - cum, -jnp.inf)
        own = jnp.sum(q * new, axis=1, keepdims=True) * scale
        top = jnp.maximum(jnp.max(scores, axis=1, keepdims=True), own)
        terms = jnp.exp(scores - top)
        own_term = jnp.exp(own - top)
        total = jnp.sum(terms, axis=1, keepdims=True) + own_term
        inverse = 1.0 / total
        probs = (terms * inverse).astype(BF16)
        prob_own = (own_term * inverse).astype(BF16).astype(F32)
        mixed = jnp.dot(probs, rows_kv, preferred_element_type=F32) + prob_own * new
        mixed_all[s] = mixed.astype(BF16).astype(F32)

    def attend_group(i, carry):
        for j in range(group):
            attend(i * group + j)
        return carry

    lax.fori_loop(0, seqs // group, attend_group, 0)

    attended = jnp.concatenate(
        [
            jnp.where(low, pltpu.roll(mixed_all[:, h, :], HEAD_DIM, 1), mixed_all[:, h + 1, :])
            for h in range(0, heads, 2)
        ],
        axis=1,
    ).astype(BF16)
    gathered = jnp.zeros((seqs, LANES), F32)
    for h in range(heads):
        gathered = jnp.where(lane == h, cum_new[:, h, :], gathered)
    new_cum_ref[...] = gathered[:, :heads]
    w_copies[3].wait()
    partial_ref[...] = jnp.dot(attended, wo[...], preferred_element_type=F32).astype(BF16)


def expert_kernel(
    ep_size,
    tp_size,
    partial_ref,
    tokens_ref,
    gain_ref,
    ids_ref,
    weight_ref,
    sg_hbm,
    su_hbm,
    sd_hbm,
    eg_hbm,
    eu_hbm,
    ed_hbm,
    out_ref,
    swgu,
    swd,
    wgu,
    wd,
    sums,
    blocks,
    parts,
    from_core,
    to_y,
    from_y,
    to_x,
    from_x,
    to_z,
    from_z,
    w_sem,
    ar_send,
    ar_recv,
    ag_recv,
    z_send,
    x_send,
    d_send,
    core_send,
    core_recv,
    yx_send,
    yx_recv,
    rz_send,
    rz_recv,
):
    seqs, width = tokens_ref.shape
    quarter = width // tp_size
    half = width // 2
    experts = eg_hbm.shape[0]
    hidden = eg_hbm.shape[2]
    nx = 2
    nz = ep_size // nx
    e = lax.axis_index("ep")
    t = lax.axis_index("tp")
    z, x = e // nx, e % nx
    y, c = t // 2, t % 2
    x_peer = z * nx + (1 - x)
    core_peer = y * 2 + (1 - c)
    y_peer = (1 - y) * 2 + c

    def slot_of(z_at, x_at):
        return x_at * nz + z_at

    def z_at(d):
        return lax.rem(z + d, nz)

    weight_copies = []
    for i in range(experts):
        weight_copies.append((eg_hbm.at[i], wgu.at[i, :, pl.ds(0, hidden)]))
        weight_copies.append((eu_hbm.at[i], wgu.at[i, :, pl.ds(hidden, hidden)]))
        weight_copies.append((ed_hbm.at[i], wd.at[pl.ds(i * hidden, hidden), :]))
    weight_copies.append((sg_hbm, swgu.at[:, pl.ds(0, hidden)]))
    weight_copies.append((su_hbm, swgu.at[:, pl.ds(hidden, hidden)]))
    weight_copies.append((sd_hbm, swd))
    weight_copies = [
        pltpu.make_async_copy(s, d, w_sem.at[i]) for i, (s, d) in enumerate(weight_copies)
    ]
    shared_copies, expert_copies = weight_copies[-3:], weight_copies[:-3]

    barrier = pltpu.get_barrier_semaphore()
    peers = [(e, lax.rem(t + k, tp_size)) for k in range(1, tp_size)]
    peers += [(z_at(d) * nx + x, t) for d in range(1, nz)]
    peers += [(x_peer, t)]
    for peer in peers:
        pl.semaphore_signal(barrier, inc=1, device_id=peer, device_id_type=MESH)
    for copy in shared_copies + expert_copies:
        copy.start()
    pl.semaphore_wait(barrier, len(peers))

    def remote(src, dst, send, recv, peer):
        return pltpu.make_async_remote_copy(
            src_ref=src,
            dst_ref=dst,
            send_sem=send,
            recv_sem=recv,
            device_id=peer,
            device_id_type=MESH,
        )

    ar_copies = [
        remote(
            partial_ref,
            sums.at[k - 1],
            ar_send.at[k - 1],
            ar_recv.at[k - 1],
            (e, lax.rem(t + k, tp_size)),
        )
        for k in range(1, tp_size)
    ]
    for copy in ar_copies:
        copy.start()
    pad = blocks.shape[3] - half
    expert_lane = lax.broadcasted_iota(jnp.int32, (seqs, pad), 1)
    dense = jnp.zeros((seqs, pad), F32)
    for k in range(ids_ref.shape[1]):
        dense += jnp.where(ids_ref[:, k : k + 1] == expert_lane, weight_ref[:, k : k + 1], 0.0)
    total = partial_ref[...].astype(F32)
    for k, copy in enumerate(ar_copies):
        copy.wait()
        total += sums[k].astype(F32)
    residual = (tokens_ref[...].astype(F32) + total).astype(BF16)
    ffn_in = rms_scale(residual, gain_ref[...]).astype(BF16)
    sums[0] = residual
    mine = slot_of(z, x)
    for h in range(2):
        blocks[mine, h, :, :half] = ffn_in[:, h * half : (h + 1) * half]
        blocks[mine, h, :, half:] = dense.astype(BF16)

    def z_copy(d, source):
        return remote(
            blocks.at[source, c],
            blocks.at[source, c],
            z_send.at[d - 1],
            ag_recv.at[source, c],
            (z_at(d) * nx + x, t),
        )

    def x_copy(source):
        return remote(
            blocks.at[source, c],
            blocks.at[source, c],
            x_send.at[source],
            ag_recv.at[source, c],
            (x_peer, t),
        )

    def d_copy(source):
        return remote(
            blocks.at[source, c],
            blocks.at[source, c],
            d_send.at[source],
            ag_recv.at[source, c],
            (e, core_peer),
        )

    def arrived(source, part):
        remote(
            blocks.at[source, part],
            blocks.at[source, part],
            d_send.at[source],
            ag_recv.at[source, part],
            (e, core_peer),
        ).wait_recv()

    x_copy(mine).start()
    for d in range(1, nz):
        z_copy(d, mine).start()

    for copy in shared_copies:
        copy.wait()
    both = jnp.dot(ffn_in, swgu[...], preferred_element_type=F32)
    shared_hidden = (jax.nn.silu(both[:, :hidden]) * both[:, hidden:]).astype(BF16)

    others_x = [slot_of(z, 1 - x)]
    arrived(others_x[0], c)
    d_copy(others_x[0]).start()
    others_z = []
    for d in range(1, nz):
        source = slot_of(lax.rem(z + nz - d, nz), x)
        others_z.append(source)
        arrived(source, c)
        x_copy(source).start()
        d_copy(source).start()
    for d in range(1, nz):
        source = slot_of(lax.rem(z + nz - d, nz), 1 - x)
        others_x.append(source)
        arrived(source, c)
        d_copy(source).start()
    for copy in expert_copies:
        copy.wait()
    for source in others_x + others_z:
        arrived(source, 1 - c)

    token_count = ep_size * seqs
    first = blocks[:, 0, :, :half].reshape(token_count, half)
    second = blocks[:, 1, :, :half].reshape(token_count, half)
    gathered = blocks[:, 0, :, half:].reshape(token_count, pad).astype(F32)
    pad_lane = lax.broadcasted_iota(jnp.int32, (token_count, pad), 1)
    pieces = []
    for i in range(experts):
        both = jnp.dot(first, wgu[i, :half, :], preferred_element_type=F32)
        both += jnp.dot(second, wgu[i, half:, :], preferred_element_type=F32)
        scale = jnp.sum(
            jnp.where(pad_lane == e * experts + i, gathered, 0.0), axis=1, keepdims=True
        )
        pieces.append((jax.nn.silu(both[:, :hidden]) * both[:, hidden:] * scale).astype(BF16))
    expert_hidden = jnp.concatenate(pieces, axis=1)

    own_rows = pl.ds(pl.multiple_of(mine * seqs, seqs), seqs)

    def column_block(index):
        return pl.ds(pl.multiple_of(index * quarter, LANES), quarter)

    core_copies = []
    for k in range(2):
        cols = column_block(2 * k + 1 - c)
        value = jnp.dot(expert_hidden, wd[:, cols], preferred_element_type=F32)
        parts[k] = value.astype(BF16)
        shared = jnp.dot(shared_hidden, swd[:, cols], preferred_element_type=F32)
        parts[k, own_rows, :] = (parts[k, own_rows, :].astype(F32) + shared).astype(BF16)
        copy = remote(
            parts.at[k], from_core.at[k], core_send.at[k], core_recv.at[k], (e, core_peer)
        )
        copy.start()
        core_copies.append(copy)

    def own_part(k, y_index):
        cols = column_block(2 * y_index + c)
        to_ref = to_y if k == 0 else to_x
        shared = jnp.dot(shared_hidden, swd[:, cols], preferred_element_type=F32)
        to_ref[...] = jnp.dot(expert_hidden, wd[:, cols], preferred_element_type=F32)
        to_ref[own_rows, :] = to_ref[own_rows, :] + shared

    own_part(0, 1 - y)
    own_part(1, y)
    for copy in core_copies:
        copy.wait()
    parts[0] = (to_y[...] + from_core[1 - y].astype(F32)).astype(BF16)
    y_copy = remote(parts.at[0], from_y, yx_send.at[0], yx_recv.at[0], (e, y_peer))
    y_copy.start()
    to_x[...] = to_x[...] + from_core[y].astype(F32)
    y_copy.wait()
    half_rows = nz * seqs
    there = pl.ds(pl.multiple_of((1 - x) * half_rows, seqs), half_rows)
    here = pl.ds(pl.multiple_of(x * half_rows, seqs), half_rows)
    parts[1, :half_rows, :] = (to_x[there, :] + from_y[there, :].astype(F32)).astype(BF16)
    x_out = remote(
        parts.at[1, pl.ds(0, half_rows)], from_x, yx_send.at[1], yx_recv.at[1], (x_peer, t)
    )
    x_out.start()
    to_y[:half_rows, :] = to_x[here, :] + from_y[here, :].astype(F32)
    x_out.wait()
    to_y[:half_rows, :] = to_y[:half_rows, :] + from_x[...].astype(F32)
    to_z[...] = to_y[:half_rows, :].astype(BF16)
    rz_copies = []
    for d in range(1, nz):
        rows = pl.ds(pl.multiple_of(z_at(d) * seqs, seqs), seqs)
        rz_copies.append(
            remote(
                to_z.at[rows],
                from_z.at[d - 1],
                rz_send.at[d - 1],
                rz_recv.at[d - 1],
                (z_at(d) * nx + x, t),
            )
        )
        rz_copies[-1].start()
    my_columns = pl.ds(pl.multiple_of(t * quarter, LANES), quarter)
    result = sums[0, :, my_columns].astype(F32)
    result += to_y[pl.ds(pl.multiple_of(z * seqs, seqs), seqs), :]
    for d, copy in enumerate(rz_copies):
        copy.wait()
        result += from_z[d].astype(F32)
    out_ref[...] = result.astype(BF16)

    for copy in [x_copy(mine)] + [z_copy(d, mine) for d in range(1, nz)]:
        copy.wait_send()
    for source in others_z:
        x_copy(source).wait_send()
    for source in others_x + others_z:
        d_copy(source).wait_send()


def shards(
    tokens,
    lengths,
    cache_kv,
    cache_cum,
    norm_attn,
    w_query,
    w_key,
    w_value,
    w_forget,
    b_forget,
    w_output,
    norm_ffn,
    shared_gate,
    shared_up,
    shared_down,
    expert_gate,
    expert_up,
    expert_down,
    route_ids,
    route_weight,
):
    ep_size = lax.axis_size("ep")
    tp_size = lax.axis_size("tp")
    seqs, width = tokens.shape
    cache_len, heads = cache_kv.shape[1], cache_kv.shape[2]
    projected = w_query.shape[1]
    columns = cache_len * heads
    head_rows = -(-heads // 8) * 8
    vmem = pl.BlockSpec(memory_space=pltpu.VMEM)
    smem = pl.BlockSpec(memory_space=pltpu.SMEM)
    anywhere = pl.BlockSpec(memory_space=pl.ANY)
    kv_rows = cache_kv.reshape(seqs, columns, 2 * HEAD_DIM)
    cum_rows = cache_cum.transpose(0, 2, 1).reshape(seqs, 1, columns)
    per_head = pltpu.VMEM((seqs, head_rows, LANES), F32)
    partial, new_kv, cum_new = pl.pallas_call(
        functools.partial(attention_kernel, 4),
        out_shape=(
            jax.ShapeDtypeStruct((seqs, width), BF16),
            jax.ShapeDtypeStruct((seqs, heads, 2 * HEAD_DIM), BF16),
            jax.ShapeDtypeStruct((seqs, heads), F32),
        ),
        in_specs=[smem] + [vmem] * 5 + [anywhere] * 5,
        out_specs=(vmem, vmem, vmem),
        scratch_shapes=[
            pltpu.VMEM((width, projected), BF16),
            pltpu.VMEM((width, projected), BF16),
            pltpu.VMEM((width, projected), BF16),
            pltpu.VMEM((projected, width), BF16),
            pltpu.VMEM((seqs, columns, 2 * HEAD_DIM), BF16),
            per_head,
            per_head,
            per_head,
            per_head,
            per_head,
            pltpu.SemaphoreType.DMA((4,)),
            pltpu.SemaphoreType.DMA((seqs,)),
        ],
        compiler_params=pltpu.CompilerParams(vmem_limit_bytes=60 * 2**20),
        name="attention",
    )(
        lengths,
        tokens,
        cum_rows,
        norm_attn.reshape(1, width),
        w_forget.T,
        b_forget.reshape(1, heads),
        w_query,
        w_key,
        w_value,
        w_output,
        kv_rows,
    )
    experts, _, hidden = expert_gate.shape
    quarter = width // tp_size
    token_count = ep_size * seqs
    nz = ep_size // 2
    pad = -(-experts * ep_size // LANES) * LANES
    dma = pltpu.SemaphoreType.DMA
    output = pl.pallas_call(
        functools.partial(expert_kernel, ep_size, tp_size),
        out_shape=jax.ShapeDtypeStruct((seqs, quarter), BF16),
        in_specs=[vmem] * 5 + [anywhere] * 6,
        out_specs=vmem,
        scratch_shapes=[
            pltpu.VMEM((width, 2 * hidden), BF16),
            pltpu.VMEM((hidden, width), BF16),
            pltpu.VMEM((experts, width, 2 * hidden), BF16),
            pltpu.VMEM((experts * hidden, width), BF16),
            pltpu.VMEM((tp_size - 1, seqs, width), BF16),
            pltpu.VMEM((ep_size, 2, seqs, width // 2 + pad), BF16),
            pltpu.VMEM((2, token_count, quarter), BF16),
            pltpu.VMEM((2, token_count, quarter), BF16),
            pltpu.VMEM((token_count, quarter), F32),
            pltpu.VMEM((token_count, quarter), BF16),
            pltpu.VMEM((token_count, quarter), F32),
            pltpu.VMEM((nz * seqs, quarter), BF16),
            pltpu.VMEM((nz * seqs, quarter), BF16),
            pltpu.VMEM((nz - 1, seqs, quarter), BF16),
            dma((3 * experts + 3,)),
            dma((tp_size - 1,)),
            dma((tp_size - 1,)),
            dma((ep_size, 2)),
            dma((nz - 1,)),
            dma((ep_size,)),
            dma((ep_size,)),
            dma((2,)),
            dma((2,)),
            dma((2,)),
            dma((2,)),
            dma((nz - 1,)),
            dma((nz - 1,)),
        ],
        compiler_params=pltpu.CompilerParams(
            collective_id=0, has_side_effects=True, vmem_limit_bytes=60 * 2**20
        ),
        name="experts",
    )(
        partial,
        tokens,
        norm_ffn.reshape(1, width),
        route_ids,
        route_weight,
        shared_gate,
        shared_up,
        shared_down,
        expert_gate,
        expert_up,
        expert_down,
    )
    return (output, new_kv, cum_new)


def shards_general(
    tokens,
    lengths,
    cache_kv,
    cache_cum,
    norm_attn,
    w_query,
    w_key,
    w_value,
    w_forget,
    b_forget,
    w_output,
    norm_ffn,
    shared_gate,
    shared_up,
    shared_down,
    expert_gate,
    expert_up,
    expert_down,
    route_ids,
    route_weight,
):
    ep_size = lax.axis_size("ep")
    tp_size = lax.axis_size("tp")
    tp_place = lax.axis_index("tp")
    seq_dev, model_width = tokens.shape
    width_part = model_width // tp_size
    heads_here = w_query.shape[1] // HEAD_DIM
    cache_len = cache_kv.shape[1]
    score_scale = HEAD_DIM ** (-0.5)
    normed = rms_scale(tokens, norm_attn).astype(jnp.bfloat16)
    queries = (
        jnp.dot(normed, w_query, preferred_element_type=jnp.float32)
        .astype(jnp.bfloat16)
        .reshape(seq_dev, heads_here, HEAD_DIM)
    )
    key_new = (
        jnp.dot(normed, w_key, preferred_element_type=jnp.float32)
        .astype(jnp.bfloat16)
        .reshape(seq_dev, heads_here, HEAD_DIM)
    )
    value_new = (
        jnp.dot(normed, w_value, preferred_element_type=jnp.float32)
        .astype(jnp.bfloat16)
        .reshape(seq_dev, heads_here, HEAD_DIM)
    )
    forget_log = jax.nn.log_sigmoid(
        jnp.dot(normed, w_forget, preferred_element_type=jnp.float32) + b_forget
    )
    last_index = jnp.broadcast_to((lengths - 1)[:, None, None], (seq_dev, heads_here, 1))
    cum_new = jnp.take_along_axis(cache_cum, last_index, axis=2)[:, :, 0] + forget_log
    past_scores = (
        jnp.einsum(
            "shd,slhd->shl",
            queries,
            cache_kv[:, :, :, :HEAD_DIM],
            preferred_element_type=jnp.float32,
        )
        * score_scale
    )
    past_scores = past_scores + cum_new[:, :, None] - cache_cum
    is_valid = jnp.arange(cache_len, dtype=jnp.int32)[None, None, :] < lengths[:, None, None]
    past_scores = jnp.where(is_valid, past_scores, -jnp.inf)
    own_score = (
        jnp.sum(queries.astype(jnp.float32) * key_new.astype(jnp.float32), axis=2) * score_scale
    )
    row_max = jnp.maximum(jnp.max(past_scores, axis=2), own_score)
    weights_past = jnp.exp(past_scores - row_max[:, :, None])
    weight_own = jnp.exp(own_score - row_max)
    weight_sum = jnp.sum(weights_past, axis=2) + weight_own
    probs_past = (weights_past / weight_sum[:, :, None]).astype(jnp.bfloat16)
    prob_own = (weight_own / weight_sum).astype(jnp.bfloat16)
    mixed = jnp.einsum(
        "shl,slhd->shd",
        probs_past,
        cache_kv[:, :, :, HEAD_DIM:],
        preferred_element_type=jnp.float32,
    )
    mixed = mixed + prob_own.astype(jnp.float32)[:, :, None] * value_new.astype(jnp.float32)
    attended = mixed.astype(jnp.bfloat16).reshape(seq_dev, heads_here * HEAD_DIM)
    partial_value = jnp.dot(attended, w_output, preferred_element_type=jnp.float32)
    summed = lax.psum(partial_value.astype(jnp.bfloat16), "tp").astype(jnp.float32)
    residual = (tokens.astype(jnp.float32) + summed).astype(jnp.bfloat16)
    ffn_in = rms_scale(residual, norm_ffn).astype(jnp.bfloat16)
    residual_part = lax.dynamic_slice_in_dim(residual, tp_place * width_part, width_part, 1)
    shared_hidden = (
        jax.nn.silu(jnp.dot(ffn_in, shared_gate, preferred_element_type=jnp.float32))
        * jnp.dot(ffn_in, shared_up, preferred_element_type=jnp.float32)
    ).astype(jnp.bfloat16)
    shared_part = jnp.dot(shared_hidden, shared_down, preferred_element_type=jnp.float32).astype(
        jnp.bfloat16
    )
    top_count = route_ids.shape[1]
    experts_here = expert_gate.shape[0]
    experts_all = experts_here * ep_size
    capacity = max(2, 2 * (seq_dev * top_count // experts_all))
    slot_count = experts_all * capacity
    route_flat = route_ids.reshape(-1)
    onehot = (route_flat[:, None] == jnp.arange(experts_all, dtype=jnp.int32)[None, :]).astype(
        jnp.int32
    )
    before = jnp.cumsum(onehot, axis=0) - onehot
    slot_rank = jnp.sum(before * onehot, axis=1)
    owner_index = route_flat // experts_here
    slot_local = route_flat % experts_here
    slot_index = ((slot_local * ep_size + owner_index) * capacity + slot_rank).reshape(
        seq_dev, top_count
    )
    slot_ids = jnp.arange(slot_count, dtype=jnp.int32)
    picker = jnp.sum(
        (slot_ids[:, None, None] == slot_index[None, :, :]).astype(jnp.bfloat16), axis=2
    )
    combine = jnp.sum(
        jnp.where(slot_ids[None, None, :] == slot_index[:, :, None], route_weight[:, :, None], 0.0),
        axis=1,
    )
    own_part = lax.dynamic_slice_in_dim(ffn_in, tp_place * width_part, width_part, 1)
    chosen = jnp.dot(picker, own_part, preferred_element_type=jnp.float32).astype(jnp.bfloat16)
    moved = lax.all_to_all(
        chosen.reshape(experts_here, ep_size, capacity, width_part),
        "ep",
        split_axis=1,
        concat_axis=1,
        tiled=True,
    )
    arrived = lax.all_gather(moved, "tp", axis=3, tiled=True)
    row_count = ep_size * capacity
    arrived = arrived.reshape(experts_here, row_count, model_width)
    gate_value = jnp.einsum(
        "erd,edf->erf", arrived, expert_gate, preferred_element_type=jnp.float32
    )
    up_value = jnp.einsum("erd,edf->erf", arrived, expert_up, preferred_element_type=jnp.float32)
    expert_hidden = (jax.nn.silu(gate_value) * up_value).astype(jnp.bfloat16)
    expert_part = jnp.einsum(
        "erf,efd->erd", expert_hidden, expert_down, preferred_element_type=jnp.float32
    ).astype(jnp.bfloat16)
    expert_pieces, shared_pieces = (
        lax.all_to_all(
            expert_part.reshape(experts_here, row_count, tp_size, width_part),
            "tp",
            split_axis=2,
            concat_axis=2,
            tiled=True,
        ),
        lax.all_to_all(
            shared_part.reshape(1, seq_dev, tp_size, width_part),
            "tp",
            split_axis=2,
            concat_axis=2,
            tiled=True,
        ),
    )
    expert_sum = jnp.sum(expert_pieces.astype(jnp.float32), axis=2).astype(jnp.bfloat16)
    shared_sum = jnp.sum(shared_pieces.astype(jnp.float32), axis=2)[0]
    returned = lax.all_to_all(
        expert_sum.reshape(experts_here, ep_size, capacity, width_part),
        "ep",
        split_axis=1,
        concat_axis=1,
        tiled=True,
    )
    routed = jnp.dot(
        combine,
        returned.reshape(slot_count, width_part).astype(jnp.float32),
        precision=lax.Precision.HIGHEST,
    )
    output = (residual_part.astype(jnp.float32) + shared_sum + routed).astype(jnp.bfloat16)
    new_kv = jnp.concatenate([key_new, value_new], axis=2)
    return (output, new_kv, cum_new)


def solution(mesh):
    in_specs = (
        P("ep", None),
        P("ep"),
        P("ep", None, "tp", None),
        P("ep", "tp", None),
        P(),
        P(None, "tp"),
        P(None, "tp"),
        P(None, "tp"),
        P(None, "tp"),
        P("tp"),
        P("tp", None),
        P(),
        P(None, "tp"),
        P(None, "tp"),
        P("tp", None),
        P("ep", None, "tp"),
        P("ep", None, "tp"),
        P("ep", "tp", None),
        P("ep", None),
        P("ep", None),
    )
    out_specs = (P("ep", "tp"), P("ep", "tp", None), P("ep", "tp"))
    fused = mesh.shape["tp"] == 4 and mesh.shape["ep"] % 2 == 0 and mesh.shape["ep"] > 2
    body = shards if fused else shards_general
    return jax.shard_map(body, mesh=mesh, in_specs=in_specs, out_specs=out_specs, check_vma=False)
```

```python
import functools

import jax
import jax.numpy as jnp
from jax import lax
from jax.experimental import pallas as pl
from jax.experimental.pallas import tpu as pltpu
from jax.sharding import PartitionSpec as P

HEAD_DIM = 64
LANES = 128
epsilon = 1e-06
MESH = pl.DeviceIdType.MESH
F32 = jnp.float32
BF16 = jnp.bfloat16


def rms_scale(row_block, gain):
    widened = row_block.astype(F32)
    return widened * lax.rsqrt(jnp.mean(widened * widened, axis=-1, keepdims=True) + epsilon) * gain


def attention_kernel(
    group,
    lengths_ref,
    tokens_ref,
    cum_ref,
    gain_ref,
    wf_ref,
    bf_ref,
    wq_hbm,
    wk_hbm,
    wv_hbm,
    wo_hbm,
    kv_hbm,
    partial_ref,
    new_kv_ref,
    new_cum_ref,
    wq,
    wk,
    wv,
    wo,
    kv,
    q_pad,
    fresh,
    forget,
    cum_new,
    mixed_all,
    w_sem,
    kv_sem,
):
    seqs = tokens_ref.shape[0]
    heads = new_kv_ref.shape[1]
    columns = kv.shape[1]
    rows = q_pad.shape[1]
    scale = HEAD_DIM ** (-0.5)
    w_copies = [
        pltpu.make_async_copy(src, dst, w_sem.at[i])
        for i, (src, dst) in enumerate(((wq_hbm, wq), (wk_hbm, wk), (wv_hbm, wv), (wo_hbm, wo)))
    ]

    def kv_copy(s):
        return pltpu.make_async_copy(kv_hbm.at[s], kv.at[s], kv_sem.at[s])

    for copy in w_copies[:3]:
        copy.start()
    for s in range(seqs):
        kv_copy(s).start()
    w_copies[3].start()

    normed = rms_scale(tokens_ref[...], gain_ref[...]).astype(BF16)
    forget_log = jax.nn.log_sigmoid(
        lax.dot_general(
            normed, wf_ref[...], (((1,), (1,)), ((), ())), preferred_element_type=F32
        )
        + bf_ref[...]
    )
    q_pad[...] = jnp.zeros_like(q_pad)
    fresh[...] = jnp.zeros_like(fresh)
    forget[...] = jnp.zeros_like(forget)
    lane = lax.broadcasted_iota(jnp.int32, (seqs, LANES), 1)
    low = lane < HEAD_DIM
    for copy in w_copies[:3]:
        copy.wait()
    queries, keys, values = (
        jnp.dot(normed, w[...], preferred_element_type=F32).astype(BF16).astype(F32)
        for w in (wq, wk, wv)
    )
    for h in range(heads):
        pair = slice((h // 2) * LANES, (h // 2 + 1) * LANES)
        q_h, k_h, v_h = queries[:, pair], keys[:, pair], values[:, pair]
        if h % 2 == 0:
            v_h = pltpu.roll(v_h, HEAD_DIM, 1)
        else:
            q_h = pltpu.roll(q_h, HEAD_DIM, 1)
            k_h = pltpu.roll(k_h, HEAD_DIM, 1)
        q_pad[:, h, :] = jnp.where(low, q_h, 0.0)
        fresh[:, h, :] = jnp.where(low, k_h, v_h)
        forget[:, h, :] = jnp.broadcast_to(forget_log[:, h : h + 1], (seqs, LANES))
    new_kv_ref[...] = fresh[:, :heads, :].astype(BF16)

    column = lax.broadcasted_iota(jnp.int32, (rows, columns), 1)
    own_head = lax.rem(column, heads) == lax.broadcasted_iota(jnp.int32, (rows, columns), 0)

    spread = lax.broadcasted_iota(jnp.int32, (rows, LANES), 1) // heads

    def attend(s):
        kv_copy(s).wait()
        length = lengths_ref[s]
        rows_kv = kv[s]
        q = q_pad[s]
        new = fresh[s]
        narrow = cum_ref[s]
        narrow = jnp.concatenate([narrow] * (rows // heads), axis=0)
        cum = jnp.concatenate(
            [
                jnp.take_along_axis(
                    narrow[:, b * LANES : (b + 1) * LANES], spread + p * (LANES // heads), axis=1
                )
                for b in range(columns // heads // LANES)
                for p in range(heads)
            ],
            axis=1,
        )
        scores = lax.dot_general(
            q.astype(BF16), rows_kv, (((1,), (1,)), ((), ())), preferred_element_type=F32
        )
        last = own_head & (column >= (length - 1) * heads) & (column < length * heads)
        cum_here = jnp.sum(jnp.where(last, cum, 0.0), axis=1, keepdims=True) + forget[s][:, :1]
        cum_new[s] = jnp.broadcast_to(cum_here, (rows, LANES))
        valid = own_head & (column < length * heads)
        scores = jnp.where(valid, scores * scale + cum_here - cum, -jnp.inf)
        own = jnp.sum(q * new, axis=1, keepdims=True) * scale
        top = jnp.maximum(jnp.max(scores, axis=1, keepdims=True), own)
        terms = jnp.exp(scores - top)
        own_term = jnp.exp(own - top)
        total = jnp.sum(terms, axis=1, keepdims=True) + own_term
        inverse = 1.0 / total
        probs = (terms * inverse).astype(BF16)
        prob_own = (own_term * inverse).astype(BF16).astype(F32)
        mixed = jnp.dot(probs, rows_kv, preferred_element_type=F32) + prob_own * new
        mixed_all[s] = mixed.astype(BF16).astype(F32)

    def attend_group(i, carry):
        for j in range(group):
            attend(i * group + j)
        return carry

    lax.fori_loop(0, seqs // group, attend_group, 0)

    attended = jnp.concatenate(
        [
            jnp.where(low, pltpu.roll(mixed_all[:, h, :], HEAD_DIM, 1), mixed_all[:, h + 1, :])
            for h in range(0, heads, 2)
        ],
        axis=1,
    ).astype(BF16)
    gathered = jnp.zeros((seqs, LANES), F32)
    for h in range(heads):
        gathered = jnp.where(lane == h, cum_new[:, h, :], gathered)
    new_cum_ref[...] = gathered.T[:heads, :]
    w_copies[3].wait()
    partial_ref[...] = jnp.dot(attended, wo[...], preferred_element_type=F32).astype(BF16)


def expert_kernel(
    ep_size,
    tp_size,
    partial_ref,
    tokens_ref,
    gain_ref,
    ids_ref,
    weight_ref,
    sg_hbm,
    su_hbm,
    sd_hbm,
    eg_hbm,
    eu_hbm,
    ed_hbm,
    out_ref,
    swgu,
    swd,
    wgu,
    wd,
    sums,
    blocks,
    parts,
    from_core,
    to_y,
    to_x,
    big_send,
    big_recv,
    small_send,
    small_recv,
    to_z,
    from_z,
    w_sem,
    ar_send,
    ar_recv,
    ag_recv,
    z_send,
    x_send,
    d_send,
    core_send,
    core_recv,
    yx_send,
    yx_recv,
    rz_send,
    rz_recv,
):
    seqs, width = tokens_ref.shape
    quarter = width // tp_size
    half = width // 2
    experts = eg_hbm.shape[0]
    hidden = eg_hbm.shape[2]
    nx = 2
    nz = ep_size // nx
    e = lax.axis_index("ep")
    t = lax.axis_index("tp")
    z, x = e // nx, e % nx
    y, c = t // 2, t % 2
    x_peer = z * nx + (1 - x)
    core_peer = y * 2 + (1 - c)
    y_peer = (1 - y) * 2 + c

    def slot_of(z_at, x_at):
        return x_at * nz + z_at

    def z_at(d):
        return lax.rem(z + d, nz)

    weight_copies = []
    for i in range(experts):
        weight_copies.append((eg_hbm.at[i], wgu.at[i, :, pl.ds(0, hidden)]))
        weight_copies.append((eu_hbm.at[i], wgu.at[i, :, pl.ds(hidden, hidden)]))
        weight_copies.append((ed_hbm.at[i], wd.at[pl.ds(i * hidden, hidden), :]))
    weight_copies.append((sg_hbm, swgu.at[:, pl.ds(0, hidden)]))
    weight_copies.append((su_hbm, swgu.at[:, pl.ds(hidden, hidden)]))
    weight_copies.append((sd_hbm, swd))
    weight_copies = [
        pltpu.make_async_copy(s, d, w_sem.at[i]) for i, (s, d) in enumerate(weight_copies)
    ]
    shared_copies, expert_copies = weight_copies[-3:], weight_copies[:-3]

    barrier = pltpu.get_barrier_semaphore()
    peers = [(e, lax.rem(t + k, tp_size)) for k in range(1, tp_size)]
    peers += [(z_at(d) * nx + x, t) for d in range(1, nz)]
    peers += [(x_peer, t)]
    for peer in peers:
        pl.semaphore_signal(barrier, inc=1, device_id=peer, device_id_type=MESH)
    for copy in shared_copies + expert_copies:
        copy.start()
    pl.semaphore_wait(barrier, len(peers))

    def remote(src, dst, send, recv, peer):
        return pltpu.make_async_remote_copy(
            src_ref=src,
            dst_ref=dst,
            send_sem=send,
            recv_sem=recv,
            device_id=peer,
            device_id_type=MESH,
        )

    ar_copies = [
        remote(
            partial_ref,
            sums.at[k - 1],
            ar_send.at[k - 1],
            ar_recv.at[k - 1],
            (e, lax.rem(t + k, tp_size)),
        )
        for k in range(1, tp_size)
    ]
    for copy in ar_copies:
        copy.start()
    pad = blocks.shape[3] - half
    expert_row = lax.broadcasted_iota(jnp.int32, (pad, seqs), 0)
    dense = jnp.zeros((pad, seqs), F32)
    for k in range(ids_ref.shape[0]):
        dense += jnp.where(ids_ref[k : k + 1, :] == expert_row, weight_ref[k : k + 1, :], 0.0)
    unit = lax.broadcasted_iota(jnp.int32, (seqs, seqs), 0) == lax.broadcasted_iota(
        jnp.int32, (seqs, seqs), 1
    )
    dense = lax.dot_general(
        jnp.where(unit, 1.0, 0.0).astype(BF16),
        dense.astype(BF16),
        (((1,), (1,)), ((), ())),
        preferred_element_type=F32,
    )
    total = partial_ref[...].astype(F32)
    for k, copy in enumerate(ar_copies):
        copy.wait()
        total += sums[k].astype(F32)
    residual = (tokens_ref[...].astype(F32) + total).astype(BF16)
    ffn_in = rms_scale(residual, gain_ref[...]).astype(BF16)
    sums[0] = residual
    mine = slot_of(z, x)
    for h in range(2):
        blocks[mine, h, :, :half] = ffn_in[:, h * half : (h + 1) * half]
        blocks[mine, h, :, half:] = dense.astype(BF16)

    def z_copy(d, source):
        return remote(
            blocks.at[source, c],
            blocks.at[source, c],
            z_send.at[d - 1],
            ag_recv.at[source, c],
            (z_at(d) * nx + x, t),
        )

    def x_copy(source):
        return remote(
            blocks.at[source, c],
            blocks.at[source, c],
            x_send.at[source],
            ag_recv.at[source, c],
            (x_peer, t),
        )

    def d_copy(source):
        return remote(
            blocks.at[source, c],
            blocks.at[source, c],
            d_send.at[source],
            ag_recv.at[source, c],
            (e, core_peer),
        )

    def arrived(source, part):
        remote(
            blocks.at[source, part],
            blocks.at[source, part],
            d_send.at[source],
            ag_recv.at[source, part],
            (e, core_peer),
        ).wait_recv()

    x_copy(mine).start()
    for d in range(1, nz):
        z_copy(d, mine).start()

    for copy in shared_copies:
        copy.wait()
    both = jnp.dot(ffn_in, swgu[...], preferred_element_type=F32)
    shared_hidden = (jax.nn.silu(both[:, :hidden]) * both[:, hidden:]).astype(BF16)

    others_x = [slot_of(z, 1 - x)]
    arrived(others_x[0], c)
    d_copy(others_x[0]).start()
    others_z = []
    for d in range(1, nz):
        source = slot_of(lax.rem(z + nz - d, nz), x)
        others_z.append(source)
        arrived(source, c)
        x_copy(source).start()
        d_copy(source).start()
    for d in range(1, nz):
        source = slot_of(lax.rem(z + nz - d, nz), 1 - x)
        others_x.append(source)
        arrived(source, c)
        d_copy(source).start()
    for copy in expert_copies:
        copy.wait()
    for source in others_x + others_z:
        arrived(source, 1 - c)

    token_count = ep_size * seqs
    first = blocks[:, 0, :, :half].reshape(token_count, half)
    second = blocks[:, 1, :, :half].reshape(token_count, half)
    gathered = blocks[:, 0, :, half:].reshape(token_count, pad).astype(F32)
    pad_lane = lax.broadcasted_iota(jnp.int32, (token_count, pad), 1)
    pieces = []
    for i in range(experts):
        both = jnp.dot(first, wgu[i, :half, :], preferred_element_type=F32)
        both += jnp.dot(second, wgu[i, half:, :], preferred_element_type=F32)
        scale = jnp.sum(
            jnp.where(pad_lane == e * experts + i, gathered, 0.0), axis=1, keepdims=True
        )
        pieces.append((jax.nn.silu(both[:, :hidden]) * both[:, hidden:] * scale).astype(BF16))
    expert_hidden = jnp.concatenate(pieces, axis=1)

    own_rows = pl.ds(pl.multiple_of(mine * seqs, seqs), seqs)

    def column_block(index):
        return pl.ds(pl.multiple_of(index * quarter, LANES), quarter)

    core_copies = []
    for k in range(2):
        cols = column_block(2 * k + 1 - c)
        value = jnp.dot(expert_hidden, wd[:, cols], preferred_element_type=F32)
        parts[k] = value.astype(BF16)
        shared = jnp.dot(shared_hidden, swd[:, cols], preferred_element_type=F32)
        parts[k, own_rows, :] = (parts[k, own_rows, :].astype(F32) + shared).astype(BF16)
        copy = remote(
            parts.at[k], from_core.at[k], core_send.at[k], core_recv.at[k], (e, core_peer)
        )
        copy.start()
        core_copies.append(copy)

    def own_part(k, y_index):
        cols = column_block(2 * y_index + c)
        to_ref = to_y if k == 0 else to_x
        shared = jnp.dot(shared_hidden, swd[:, cols], preferred_element_type=F32)
        to_ref[...] = jnp.dot(expert_hidden, wd[:, cols], preferred_element_type=F32)
        to_ref[own_rows, :] = to_ref[own_rows, :] + shared

    own_part(0, 1 - y)
    own_part(1, y)
    for copy in core_copies:
        copy.wait()
    half_rows = nz * seqs
    cut = quarter // 2
    there = pl.ds(pl.multiple_of((1 - x) * half_rows, seqs), half_rows)
    here = pl.ds(pl.multiple_of(x * half_rows, seqs), half_rows)

    def exchange(src, dst, k, peer):
        copy = remote(src, dst, yx_send.at[k], yx_recv.at[k], peer)
        copy.start()
        return copy

    to_y[...] = to_y[...] + from_core[1 - y].astype(F32)
    big_send[0] = to_y[:, :cut].astype(BF16)
    first_y = exchange(big_send.at[0], big_recv.at[0], 0, (e, y_peer))
    to_x[...] = to_x[...] + from_core[y].astype(F32)
    big_send[1, :half_rows, :] = to_y[there, cut:].astype(BF16)
    big_send[1, half_rows:, :] = to_x[there, cut:].astype(BF16)
    first_x = exchange(big_send.at[1], big_recv.at[1], 1, (x_peer, t))
    first_y.wait()
    to_x[:, :cut] = to_x[:, :cut] + big_recv[0].astype(F32)
    small_send[0] = to_x[there, :cut].astype(BF16)
    second_x = exchange(small_send.at[0], small_recv.at[0], 2, (x_peer, t))
    first_x.wait()
    small_send[1] = (to_y[here, cut:] + big_recv[1, :half_rows, :].astype(F32)).astype(BF16)
    second_y = exchange(small_send.at[1], small_recv.at[1], 3, (e, y_peer))
    right = to_x[here, cut:] + big_recv[1, half_rows:, :].astype(F32)
    second_x.wait()
    to_y[:half_rows, :cut] = to_x[here, :cut] + small_recv[0].astype(F32)
    second_y.wait()
    to_y[:half_rows, cut:] = right + small_recv[1].astype(F32)
    to_z[...] = to_y[:half_rows, :].astype(BF16)
    rz_copies = []
    for d in range(1, nz):
        rows = pl.ds(pl.multiple_of(z_at(d) * seqs, seqs), seqs)
        rz_copies.append(
            remote(
                to_z.at[rows],
                from_z.at[d - 1],
                rz_send.at[d - 1],
                rz_recv.at[d - 1],
                (z_at(d) * nx + x, t),
            )
        )
        rz_copies[-1].start()
    my_columns = pl.ds(pl.multiple_of(t * quarter, LANES), quarter)
    result = sums[0, :, my_columns].astype(F32)
    result += to_y[pl.ds(pl.multiple_of(z * seqs, seqs), seqs), :]
    for d, copy in enumerate(rz_copies):
        copy.wait()
        result += from_z[d].astype(F32)
    out_ref[...] = result.astype(BF16)

    for copy in [x_copy(mine)] + [z_copy(d, mine) for d in range(1, nz)]:
        copy.wait_send()
    for source in others_z:
        x_copy(source).wait_send()
    for source in others_x + others_z:
        d_copy(source).wait_send()


def shards(
    tokens,
    lengths,
    cache_kv,
    cache_cum,
    norm_attn,
    w_query,
    w_key,
    w_value,
    w_forget,
    b_forget,
    w_output,
    norm_ffn,
    shared_gate,
    shared_up,
    shared_down,
    expert_gate,
    expert_up,
    expert_down,
    route_ids,
    route_weight,
):
    ep_size = lax.axis_size("ep")
    tp_size = lax.axis_size("tp")
    seqs, width = tokens.shape
    cache_len, heads = cache_kv.shape[1], cache_kv.shape[2]
    projected = w_query.shape[1]
    columns = cache_len * heads
    head_rows = -(-heads // 8) * 8
    vmem = pl.BlockSpec(memory_space=pltpu.VMEM)
    smem = pl.BlockSpec(memory_space=pltpu.SMEM)
    anywhere = pl.BlockSpec(memory_space=pl.ANY)
    kv_rows = cache_kv.reshape(seqs, columns, 2 * HEAD_DIM)
    per_head = pltpu.VMEM((seqs, head_rows, LANES), F32)
    partial, new_kv, cum_new = pl.pallas_call(
        functools.partial(attention_kernel, 4),
        out_shape=(
            jax.ShapeDtypeStruct((seqs, width), BF16),
            jax.ShapeDtypeStruct((seqs, heads, 2 * HEAD_DIM), BF16),
            jax.ShapeDtypeStruct((heads, seqs), F32),
        ),
        in_specs=[smem] + [vmem] * 5 + [anywhere] * 5,
        out_specs=(vmem, vmem, vmem),
        scratch_shapes=[
            pltpu.VMEM((width, projected), BF16),
            pltpu.VMEM((width, projected), BF16),
            pltpu.VMEM((width, projected), BF16),
            pltpu.VMEM((projected, width), BF16),
            pltpu.VMEM((seqs, columns, 2 * HEAD_DIM), BF16),
            per_head,
            per_head,
            per_head,
            per_head,
            per_head,
            pltpu.SemaphoreType.DMA((4,)),
            pltpu.SemaphoreType.DMA((seqs,)),
        ],
        compiler_params=pltpu.CompilerParams(vmem_limit_bytes=60 * 2**20),
        name="attention",
    )(
        lengths,
        tokens,
        cache_cum,
        norm_attn.reshape(1, width),
        w_forget.T,
        b_forget.reshape(1, heads),
        w_query,
        w_key,
        w_value,
        w_output,
        kv_rows,
    )
    experts, _, hidden = expert_gate.shape
    quarter = width // tp_size
    token_count = ep_size * seqs
    nz = ep_size // 2
    pad = -(-experts * ep_size // LANES) * LANES
    dma = pltpu.SemaphoreType.DMA
    output = pl.pallas_call(
        functools.partial(expert_kernel, ep_size, tp_size),
        out_shape=jax.ShapeDtypeStruct((seqs, quarter), BF16),
        in_specs=[vmem] * 5 + [anywhere] * 6,
        out_specs=vmem,
        scratch_shapes=[
            pltpu.VMEM((width, 2 * hidden), BF16),
            pltpu.VMEM((hidden, width), BF16),
            pltpu.VMEM((experts, width, 2 * hidden), BF16),
            pltpu.VMEM((experts * hidden, width), BF16),
            pltpu.VMEM((tp_size - 1, seqs, width), BF16),
            pltpu.VMEM((ep_size, 2, seqs, width // 2 + pad), BF16),
            pltpu.VMEM((2, token_count, quarter), BF16),
            pltpu.VMEM((2, token_count, quarter), BF16),
            pltpu.VMEM((token_count, quarter), F32),
            pltpu.VMEM((token_count, quarter), F32),
            pltpu.VMEM((2, token_count, quarter // 2), BF16),
            pltpu.VMEM((2, token_count, quarter // 2), BF16),
            pltpu.VMEM((2, nz * seqs, quarter // 2), BF16),
            pltpu.VMEM((2, nz * seqs, quarter // 2), BF16),
            pltpu.VMEM((nz * seqs, quarter), BF16),
            pltpu.VMEM((nz - 1, seqs, quarter), BF16),
            dma((3 * experts + 3,)),
            dma((tp_size - 1,)),
            dma((tp_size - 1,)),
            dma((ep_size, 2)),
            dma((nz - 1,)),
            dma((ep_size,)),
            dma((ep_size,)),
            dma((2,)),
            dma((2,)),
            dma((4,)),
            dma((4,)),
            dma((nz - 1,)),
            dma((nz - 1,)),
        ],
        compiler_params=pltpu.CompilerParams(
            collective_id=0, has_side_effects=True, vmem_limit_bytes=60 * 2**20
        ),
        name="experts",
    )(
        partial,
        tokens,
        norm_ffn.reshape(1, width),
        route_ids.T,
        route_weight.T,
        shared_gate,
        shared_up,
        shared_down,
        expert_gate,
        expert_up,
        expert_down,
    )
    return (output, new_kv, cum_new.T)


def shards_general(
    tokens,
    lengths,
    cache_kv,
    cache_cum,
    norm_attn,
    w_query,
    w_key,
    w_value,
    w_forget,
    b_forget,
    w_output,
    norm_ffn,
    shared_gate,
    shared_up,
    shared_down,
    expert_gate,
    expert_up,
    expert_down,
    route_ids,
    route_weight,
):
    ep_size = lax.axis_size("ep")
    tp_size = lax.axis_size("tp")
    tp_place = lax.axis_index("tp")
    seq_dev, model_width = tokens.shape
    width_part = model_width // tp_size
    heads_here = w_query.shape[1] // HEAD_DIM
    cache_len = cache_kv.shape[1]
    score_scale = HEAD_DIM ** (-0.5)
    normed = rms_scale(tokens, norm_attn).astype(jnp.bfloat16)
    queries = (
        jnp.dot(normed, w_query, preferred_element_type=jnp.float32)
        .astype(jnp.bfloat16)
        .reshape(seq_dev, heads_here, HEAD_DIM)
    )
    key_new = (
        jnp.dot(normed, w_key, preferred_element_type=jnp.float32)
        .astype(jnp.bfloat16)
        .reshape(seq_dev, heads_here, HEAD_DIM)
    )
    value_new = (
        jnp.dot(normed, w_value, preferred_element_type=jnp.float32)
        .astype(jnp.bfloat16)
        .reshape(seq_dev, heads_here, HEAD_DIM)
    )
    forget_log = jax.nn.log_sigmoid(
        jnp.dot(normed, w_forget, preferred_element_type=jnp.float32) + b_forget
    )
    last_index = jnp.broadcast_to((lengths - 1)[:, None, None], (seq_dev, heads_here, 1))
    cum_new = jnp.take_along_axis(cache_cum, last_index, axis=2)[:, :, 0] + forget_log
    past_scores = (
        jnp.einsum(
            "shd,slhd->shl",
            queries,
            cache_kv[:, :, :, :HEAD_DIM],
            preferred_element_type=jnp.float32,
        )
        * score_scale
    )
    past_scores = past_scores + cum_new[:, :, None] - cache_cum
    is_valid = jnp.arange(cache_len, dtype=jnp.int32)[None, None, :] < lengths[:, None, None]
    past_scores = jnp.where(is_valid, past_scores, -jnp.inf)
    own_score = (
        jnp.sum(queries.astype(jnp.float32) * key_new.astype(jnp.float32), axis=2) * score_scale
    )
    row_max = jnp.maximum(jnp.max(past_scores, axis=2), own_score)
    weights_past = jnp.exp(past_scores - row_max[:, :, None])
    weight_own = jnp.exp(own_score - row_max)
    weight_sum = jnp.sum(weights_past, axis=2) + weight_own
    probs_past = (weights_past / weight_sum[:, :, None]).astype(jnp.bfloat16)
    prob_own = (weight_own / weight_sum).astype(jnp.bfloat16)
    mixed = jnp.einsum(
        "shl,slhd->shd",
        probs_past,
        cache_kv[:, :, :, HEAD_DIM:],
        preferred_element_type=jnp.float32,
    )
    mixed = mixed + prob_own.astype(jnp.float32)[:, :, None] * value_new.astype(jnp.float32)
    attended = mixed.astype(jnp.bfloat16).reshape(seq_dev, heads_here * HEAD_DIM)
    partial_value = jnp.dot(attended, w_output, preferred_element_type=jnp.float32)
    summed = lax.psum(partial_value.astype(jnp.bfloat16), "tp").astype(jnp.float32)
    residual = (tokens.astype(jnp.float32) + summed).astype(jnp.bfloat16)
    ffn_in = rms_scale(residual, norm_ffn).astype(jnp.bfloat16)
    residual_part = lax.dynamic_slice_in_dim(residual, tp_place * width_part, width_part, 1)
    shared_hidden = (
        jax.nn.silu(jnp.dot(ffn_in, shared_gate, preferred_element_type=jnp.float32))
        * jnp.dot(ffn_in, shared_up, preferred_element_type=jnp.float32)
    ).astype(jnp.bfloat16)
    shared_part = jnp.dot(shared_hidden, shared_down, preferred_element_type=jnp.float32).astype(
        jnp.bfloat16
    )
    top_count = route_ids.shape[1]
    experts_here = expert_gate.shape[0]
    experts_all = experts_here * ep_size
    capacity = max(2, 2 * (seq_dev * top_count // experts_all))
    slot_count = experts_all * capacity
    route_flat = route_ids.reshape(-1)
    onehot = (route_flat[:, None] == jnp.arange(experts_all, dtype=jnp.int32)[None, :]).astype(
        jnp.int32
    )
    before = jnp.cumsum(onehot, axis=0) - onehot
    slot_rank = jnp.sum(before * onehot, axis=1)
    owner_index = route_flat // experts_here
    slot_local = route_flat % experts_here
    slot_index = ((slot_local * ep_size + owner_index) * capacity + slot_rank).reshape(
        seq_dev, top_count
    )
    slot_ids = jnp.arange(slot_count, dtype=jnp.int32)
    picker = jnp.sum(
        (slot_ids[:, None, None] == slot_index[None, :, :]).astype(jnp.bfloat16), axis=2
    )
    combine = jnp.sum(
        jnp.where(slot_ids[None, None, :] == slot_index[:, :, None], route_weight[:, :, None], 0.0),
        axis=1,
    )
    own_part = lax.dynamic_slice_in_dim(ffn_in, tp_place * width_part, width_part, 1)
    chosen = jnp.dot(picker, own_part, preferred_element_type=jnp.float32).astype(jnp.bfloat16)
    moved = lax.all_to_all(
        chosen.reshape(experts_here, ep_size, capacity, width_part),
        "ep",
        split_axis=1,
        concat_axis=1,
        tiled=True,
    )
    arrived = lax.all_gather(moved, "tp", axis=3, tiled=True)
    row_count = ep_size * capacity
    arrived = arrived.reshape(experts_here, row_count, model_width)
    gate_value = jnp.einsum(
        "erd,edf->erf", arrived, expert_gate, preferred_element_type=jnp.float32
    )
    up_value = jnp.einsum("erd,edf->erf", arrived, expert_up, preferred_element_type=jnp.float32)
    expert_hidden = (jax.nn.silu(gate_value) * up_value).astype(jnp.bfloat16)
    expert_part = jnp.einsum(
        "erf,efd->erd", expert_hidden, expert_down, preferred_element_type=jnp.float32
    ).astype(jnp.bfloat16)
    expert_pieces, shared_pieces = (
        lax.all_to_all(
            expert_part.reshape(experts_here, row_count, tp_size, width_part),
            "tp",
            split_axis=2,
            concat_axis=2,
            tiled=True,
        ),
        lax.all_to_all(
            shared_part.reshape(1, seq_dev, tp_size, width_part),
            "tp",
            split_axis=2,
            concat_axis=2,
            tiled=True,
        ),
    )
    expert_sum = jnp.sum(expert_pieces.astype(jnp.float32), axis=2).astype(jnp.bfloat16)
    shared_sum = jnp.sum(shared_pieces.astype(jnp.float32), axis=2)[0]
    returned = lax.all_to_all(
        expert_sum.reshape(experts_here, ep_size, capacity, width_part),
        "ep",
        split_axis=1,
        concat_axis=1,
        tiled=True,
    )
    routed = jnp.dot(
        combine,
        returned.reshape(slot_count, width_part).astype(jnp.float32),
        precision=lax.Precision.HIGHEST,
    )
    output = (residual_part.astype(jnp.float32) + shared_sum + routed).astype(jnp.bfloat16)
    new_kv = jnp.concatenate([key_new, value_new], axis=2)
    return (output, new_kv, cum_new)


def solution(mesh):
    in_specs = (
        P("ep", None),
        P("ep"),
        P("ep", None, "tp", None),
        P("ep", "tp", None),
        P(),
        P(None, "tp"),
        P(None, "tp"),
        P(None, "tp"),
        P(None, "tp"),
        P("tp"),
        P("tp", None),
        P(),
        P(None, "tp"),
        P(None, "tp"),
        P("tp", None),
        P("ep", None, "tp"),
        P("ep", None, "tp"),
        P("ep", "tp", None),
        P("ep", None),
        P("ep", None),
    )
    out_specs = (P("ep", "tp"), P("ep", "tp", None), P("ep", "tp"))
    fused = mesh.shape["tp"] == 4 and mesh.shape["ep"] % 2 == 0 and mesh.shape["ep"] > 2
    body = shards if fused else shards_general
    return jax.shard_map(body, mesh=mesh, in_specs=in_specs, out_specs=out_specs, check_vma=False)
```
